32 devices in a mesh: grp: 2 (over y), sp: 4 (over z), tp: 4 (over x, core).
Axes of the slice: x: 2, y: 2, z: 4, core: 2. Of those that a mesh axis runs over, the one named last changes fastest.
Arguments:
- resid: bfloat16 [4096, 2048], P(('grp', 'sp', 'tp')), parts along dimension 0, may hold values from -6 to 6
- pool_input: bfloat16 [4096, 512], P(('grp', 'sp'), 'tp'), parts along dimension 0, may hold values from -6 to 6
- group_map: bfloat16 [4, 128, 128], P('tp'), may hold values from -0.5 to 0.5
- pool_scale: bfloat16 [512], P('tp'), may hold values from 0.099609375 to 1.8984375
- out_proj: bfloat16 [512, 2048], P('tp'), may hold values from -0.25 to 0.25
- norm_gain: bfloat16 [2048], replicated, may hold values from 0.099609375 to 1.8984375
- routes: int32 [4096, 2], P(('grp', 'sp', 'tp')), parts along dimension 0, may hold values from 0 to 3, all different within a row; in each aligned block of 128 rows (0 to 127, 128 to 255, ...) at most 80 rows name the same one
- route_weight: float32 [4096, 2], P(('grp', 'sp', 'tp')), parts along dimension 0, may hold values from 0.2 to 1
- expert_gate: bfloat16 [4, 2048, 3584], P('sp', None, 'tp'), may hold values from -0.125 to 0.125
- expert_up: bfloat16 [4, 2048, 3584], P('sp', None, 'tp'), may hold values from -0.125 to 0.125
- expert_down: bfloat16 [4, 3584, 2048], P('sp', 'tp'), may hold values from -0.09375 to 0.09375
Outputs:
- layer_out: bfloat16 [4096, 2048], P(('grp', 'sp', 'tp')), parts along dimension 0
The draws below stay inside these ranges and needn't reach their ends.
There are 2 independent parts, one for each index of `grp`. The reference program is written for one: setup_inputs(seed, part) draws one part's arguments, and reference() takes and returns one part's arrays. A program takes and returns all parts, laid end to end along the dimension named above; an argument that names none is the same for every part. Nothing has to cross between parts.
Inputs may be any that keep to these rules, and one draw needn't show every extreme that they name: The 2 routes of a token differ. Among the tokens of one device (aligned blocks of 128 tokens), no expert is named more than 80 times, and in every draw some device names some expert exactly 80 times.
All inputs are finite; a program needn't handle non-finite values.
Results may differ from the reference program's by a relative error of at most 0.011.
Values may be sent and summed in bfloat16 or wider, within the bound.
No kernel may reach another device: no remote copies, remote signals or barrier semaphores. Data moves between devices by JAX's collectives and lax.ppermute only.
A program may use at most 128 MiB of HBM per device.

```python
import math
import jax
import jax.numpy as jnp
import numpy as np
from jax import lax

D = 2048
GROUPS = 4
POOL_WIDTH = 512
GROUP_DIM = 128
EXPERT_FF = 3584
TOPK = 2
EXPERTS = 4
ROWS_DEV = 128
TOKENS = 2048
CAP = 80
N_SP = 4
N_TP = 4


def levels(key, dims, split, low, top_value):
    loudness = 1.0
    for position, blocks in split:
        steps = jax.random.uniform(jax.random.fold_in(jax.random.fold_in(key, 6), position), (blocks,), jnp.float32, low / len(split), top_value / len(split))
        loudness = loudness * jnp.repeat(jnp.exp(steps), dims[position] // blocks).reshape((-1,) + (1,) * (len(dims) - 1 - position))
    return loudness


def deal_out(own_key, own, number, rows, count, top, most, lean):
    sequence = jax.random.permutation(own_key, count)
    crowded, common = portions_of(count, rows * top, most, lean, True), portions_of(count, rows * top, most, lean, False)
    places = jnp.arange(count)

    def named(sizes, rotation):
        used = int((sizes > 0).sum())
        fixed = max(1, used // 4)
        shifted = fixed + (places - fixed + rotation * (used - fixed)) % max(1, count - fixed)
        return jnp.zeros((count,), jnp.int32).at[sequence[jnp.where(places < fixed, places, shifted)]].set(jnp.asarray(sizes, jnp.int32))

    sizes = jnp.where(number % 4 == 0, named(crowded, number // 4), named(common, number - number // 4 - 1))
    mixed = jax.random.permutation(jax.random.fold_in(own, 3), count)
    source_of, taker = mixed[0:count // 2 * 2:2], mixed[1:count // 2 * 2:2]
    slack = jnp.minimum(sizes[source_of] - 1, most - sizes[taker]) // 2
    slack = jnp.where((source_of == sequence[0]) | (taker == sequence[0]) | (sizes[taker] == 0), 0, jnp.maximum(slack, 0))
    shifted = jax.random.randint(jax.random.fold_in(own, 4), (count // 2,), 0, 1 << 20) % (slack + 1)
    sizes = sizes.at[source_of].add(-shifted).at[taker].add(shifted)
    members = jnp.searchsorted(jnp.cumsum(sizes), jnp.arange(rows * top), side="right").astype(jnp.int32)
    grid = members.reshape(top, rows).T
    grid = grid[jax.random.permutation(jax.random.fold_in(own, 1), rows)]
    rotation = jax.random.randint(jax.random.fold_in(own, 2), (rows, 1), 0, top)
    return jnp.take_along_axis(grid, (jnp.arange(top)[None, :] + rotation) % top, axis=1)


def portions_of(amount, total, reach, lean, full):
    portions = [(1 << 20) // math.isqrt(grade ** lean) + 1 for grade in range(1, amount + 1)]
    largest = reach if full else min(reach, max(-(-total // amount), total * portions[0] // sum(portions)))
    least = 1 if total - largest >= amount - 1 else 0
    counts, rest = [largest] + [least] * (amount - 1), total - largest - least * (amount - 1)
    while rest > 0:
        candidates = [i for i in range(1, amount) if counts[i] < largest] or [i for i in range(1, amount) if counts[i] < reach]
        mass, remaining = sum([portions[i] for i in candidates]), rest
        for i in candidates:
            more = min(reach - counts[i], max(1, remaining * portions[i] // mass), rest)
            counts[i] = counts[i] + more
            rest = rest - more
    return np.array(counts)


def bell_draw(key, shape, spread, limit, cuts=(), kind=jnp.bfloat16):
    result = spread * jax.random.normal(key, shape, jnp.float32)
    if cuts:
        result = result * levels(key, shape, cuts, -0.22, 0.18)
    return jnp.clip(result, -limit, limit).astype(kind)


def setup_inputs(seed: int = 0, part: int = 0) -> dict:
    keys = jax.random.split(jax.random.key(seed), 12)
    part_splits = jax.random.split(jax.random.fold_in(keys[11], part), 12)
    resid = bell_draw(part_splits[0], (TOKENS, D), 1.0, 6.0, ((0, 16),))
    pool_input = bell_draw(part_splits[1], (TOKENS, POOL_WIDTH), 1.0, 6.0, ((0, 4), (1, 4)))
    group_map = bell_draw(keys[2], (GROUPS, GROUP_DIM, GROUP_DIM), GROUP_DIM ** -0.5, 0.5, ((0, 4),))
    pool_scale = jnp.clip(1.0 + 0.18 * jax.random.normal(keys[3], (POOL_WIDTH,), jnp.float32), 0.099609375, 1.8984375).astype(jnp.bfloat16)
    out_proj = bell_draw(keys[4], (POOL_WIDTH, D), POOL_WIDTH ** -0.5, 0.25, ((0, 4),))
    norm_gain = jnp.clip(1.0 + 0.18 * jax.random.normal(keys[5], (D,), jnp.float32), 0.099609375, 1.8984375).astype(jnp.bfloat16)
    routes_keys = jax.random.split(jax.random.fold_in(part_splits[6], 1), TOKENS // ROWS_DEV)
    routes_turns = jax.random.permutation(jax.random.fold_in(part_splits[6], 3), TOKENS // ROWS_DEV)
    routes = jax.vmap(lambda own, number: deal_out(jax.random.fold_in(part_splits[6], 2), own, number, ROWS_DEV, EXPERTS, TOPK, CAP, 1))(routes_keys, routes_turns).reshape((TOKENS, TOPK))
    route_weight = jnp.clip(0.2 + 0.8 * jax.random.uniform(part_splits[7], (TOKENS, TOPK), jnp.float32) ** levels(part_splits[7], (TOKENS, TOPK), ((0, 16),), -0.2, 0.2), 0.2, 1.0)
    expert_gate = bell_draw(keys[8], (EXPERTS, D, EXPERT_FF), D ** -0.5, 0.125, ((0, 4), (2, 4)))
    expert_up = bell_draw(keys[9], (EXPERTS, D, EXPERT_FF), D ** -0.5, 0.125, ((0, 4), (2, 4)))
    expert_down = bell_draw(keys[10], (EXPERTS, EXPERT_FF, D), EXPERT_FF ** -0.5, 0.09375, ((0, 4), (1, 4)))
    return {"resid": resid, "pool_input": pool_input, "group_map": group_map, "pool_scale": pool_scale, "out_proj": out_proj, "norm_gain": norm_gain, "routes": routes, "route_weight": route_weight, "expert_gate": expert_gate, "expert_up": expert_up, "expert_down": expert_down}


norm_eps = 1e-06

def pool_group(values, window):
    window_sum = values
    for back in range(1, window):
        window_sum = window_sum + jnp.pad(values[:-back], ((back, 0), (0, 0)))
    divisor = jnp.minimum(jnp.arange(1, values.shape[0] + 1, dtype=jnp.float32), jnp.float32(window))
    return (window_sum / divisor[:, None] - values).astype(jnp.bfloat16)

def reference(resid, pool_input, group_map, pool_scale, out_proj, norm_gain, routes, route_weight, expert_gate, expert_up, expert_down):
    values = pool_input.astype(jnp.float32)
    pieces = []
    for group in range(GROUPS):
        low = group * GROUP_DIM
        pooled = pool_group(values[:, low:low + GROUP_DIM], 2 ** (group + 1))
        product = jnp.dot(pooled, group_map[group], preferred_element_type=jnp.float32)
        pieces.append((product * pool_scale[low:low + GROUP_DIM].astype(jnp.float32)).astype(jnp.bfloat16))
    group_out = jnp.concatenate(pieces, axis=1)
    mix = jnp.dot(group_out, out_proj, preferred_element_type=jnp.float32)
    mixed = (resid.astype(jnp.float32) + mix).astype(jnp.bfloat16)
    residual = mixed.astype(jnp.float32)
    scaled = residual * lax.rsqrt(lax.optimization_barrier(jnp.mean(residual * residual, axis=1, keepdims=True)) + norm_eps)
    normed = (scaled * norm_gain.astype(jnp.float32)).astype(jnp.bfloat16)
    flat_routes = routes.reshape(-1).astype(jnp.int32)
    flat_rows = jnp.repeat(normed, TOPK, axis=0)
    buffer_rows = N_SP * N_TP * CAP
    quarter = EXPERT_FF // N_TP

    def per_expert(carry, expert):
        chosen = flat_routes == expert
        rank = (jnp.cumsum(chosen.astype(jnp.int32)) - 1).astype(jnp.int32)
        place = jnp.where(chosen, rank, buffer_rows).astype(jnp.int32)
        buffer = jnp.zeros((buffer_rows, D), jnp.bfloat16).at[place].set(flat_rows, mode='drop')
        gate = jnp.dot(buffer, expert_gate[expert], preferred_element_type=jnp.float32)
        up_value = jnp.dot(buffer, expert_up[expert], preferred_element_type=jnp.float32)
        hidden = (jax.nn.silu(gate) * up_value).astype(jnp.bfloat16)
        down_w = expert_down[expert]
        output = jnp.zeros((buffer_rows, D), jnp.float32)
        for lane in range(N_TP):
            partial_out = jnp.dot(hidden[:, lane * quarter:(lane + 1) * quarter], down_w[lane * quarter:(lane + 1) * quarter], preferred_element_type=jnp.float32)
            output = output + lax.optimization_barrier(partial_out.astype(jnp.bfloat16)).astype(jnp.float32)
        picked = jnp.take(output, jnp.minimum(place, buffer_rows - 1), axis=0)
        return (carry + jnp.where(chosen[:, None], picked, jnp.float32(0.0)), None)
    routed, _ = lax.scan(per_expert, jnp.zeros((TOKENS * TOPK, D), jnp.float32), jnp.arange(EXPERTS, dtype=jnp.int32))
    moe = lax.optimization_barrier(jnp.sum(routed.reshape(TOKENS, TOPK, D) * route_weight.astype(jnp.float32)[:, :, None], axis=1))
    return (residual + moe).astype(jnp.bfloat16)
```

```python
import jax
import jax.numpy as jnp
from jax import lax
from jax.experimental import pallas as pl
from jax.experimental.pallas import tpu as pltpu
from jax.sharding import PartitionSpec as P

GROUPS = 4


norm_eps = 1e-06


def from_behind(value, axis, steps):
    count = lax.axis_size(axis)
    leading, last = (max(0, -steps), min(count, count - steps))
    return lax.ppermute(value, axis, [(source, source + steps) for source in range(leading, last)])


def around(value, axis, steps):
    count = lax.axis_size(axis)
    return lax.ppermute(value, axis, [(source, (source + steps) % count) for source in range(count)])


def across(value, axis, bit):
    count = lax.axis_size(axis)
    return lax.ppermute(value, axis, [(source, source ^ bit) for source in range(count)])


def expert_block(parts, gate_w, up_w, down_w):
    rows = jnp.concatenate(parts, axis=0)
    gate = jnp.dot(rows, gate_w, preferred_element_type=jnp.float32)
    up_value = jnp.dot(rows, up_w, preferred_element_type=jnp.float32)
    hidden = (jax.nn.silu(gate) * up_value).astype(jnp.bfloat16)
    value = jnp.dot(hidden, down_w, preferred_element_type=jnp.float32).astype(jnp.bfloat16)
    slots = parts[0].shape[0]
    half = value.shape[0] // 2
    return value[:slots], value[slots:half], value[half:]


def expert_kernel(parts, gate_w, up_w, down_w):
    count = len(parts)
    slots, width = parts[0].shape
    units = gate_w.shape[1]
    rows = count * slots
    half = rows // 2
    tile = 256
    cuts = [(start, min(tile, units - start)) for start in range(0, units, tile)]

    def body(*refs):
        ins = refs[:count]
        gate, up, down = refs[count : count + 3]
        own, other, send = refs[count + 3 : count + 6]
        x, hidden = refs[count + 6 :]
        for n in range(count):
            x[n * slots : (n + 1) * slots, :] = ins[n][...]
        for start, size in cuts:
            g = jnp.dot(x[...], gate[:, start : start + size], preferred_element_type=jnp.float32)
            u = jnp.dot(x[...], up[:, start : start + size], preferred_element_type=jnp.float32)
            hidden[:, start : start + size] = (g / (1.0 + jnp.exp(-g)) * u).astype(jnp.bfloat16)
        value = jnp.dot(hidden[...], down[...], preferred_element_type=jnp.float32)
        value = value.astype(jnp.bfloat16)
        own[...] = value[:slots]
        other[...] = value[slots:half]
        send[...] = value[half:]

    whole = pl.BlockSpec(memory_space=pltpu.VMEM)
    return pl.pallas_call(
        body,
        out_shape=(
            jax.ShapeDtypeStruct((slots, width), jnp.bfloat16),
            jax.ShapeDtypeStruct((half - slots, width), jnp.bfloat16),
            jax.ShapeDtypeStruct((rows - half, width), jnp.bfloat16),
        ),
        in_specs=[whole] * (count + 3),
        out_specs=(whole,) * 3,
        scratch_shapes=[
            pltpu.VMEM((rows, width), jnp.bfloat16),
            pltpu.VMEM((rows, units), jnp.bfloat16),
        ],
        compiler_params=pltpu.CompilerParams(vmem_limit_bytes=30 * 2**20),
        cost_estimate=pl.CostEstimate(
            flops=6 * rows * width * units,
            bytes_accessed=2 * rows * width * 2,
            transcendentals=rows * units,
        ),
        name="experts",
    )(*parts, gate_w, up_w, down_w)


def pieces_of(pool_input, group_map, pool_scale):
    seq_rows = pool_input.shape[0]
    reach = 2**GROUPS - 1
    rim_rows = from_behind(pool_input[seq_rows - reach :], "sp", 1)
    extended = jnp.concatenate([rim_rows, pool_input], axis=0).astype(jnp.float32)
    positions = lax.axis_index("sp") * seq_rows + jnp.arange(1, seq_rows + 1, dtype=jnp.int32)
    group = lax.axis_index("tp") * group_map.shape[0]
    window = jnp.left_shift(jnp.int32(2), group)
    window_sum = jnp.zeros((seq_rows, group_map.shape[1]), jnp.float32)
    for back in range(reach + 1):
        window_sum = window_sum + jnp.where(
            back < window, extended[reach - back : reach - back + seq_rows], jnp.float32(0.0)
        )
    divisor = jnp.minimum(positions, window).astype(jnp.float32)
    pooled = (window_sum / divisor[:, None] - extended[reach:]).astype(jnp.bfloat16)
    product = jnp.dot(pooled, group_map[0], preferred_element_type=jnp.float32)
    return (product * pool_scale.astype(jnp.float32)).astype(jnp.bfloat16)


def hypercube(held, axis):
    bit = lax.axis_size(axis) // 2
    while bit:
        held = held + [across(value, axis, bit) for value in held]
        bit //= 2
    return held


def local(
    resid,
    pool_input,
    group_map,
    pool_scale,
    out_proj,
    norm_gain,
    routes,
    route_weight,
    expert_gate,
    expert_up,
    expert_down,
):
    own_rows, width = resid.shape
    lanes = lax.axis_size("tp")
    steps = lax.axis_size("sp")
    top_count = routes.shape[1]
    experts = steps * expert_gate.shape[0]
    slots = max(2, 5 * own_rows * top_count // (4 * experts))
    lane = lax.axis_index("tp")
    relative = [0]
    bit = lanes // 2
    while bit:
        relative = relative + [r ^ bit for r in relative]
        bit //= 2

    projections = hypercube([out_proj], "tp")
    pieces = pieces_of(pool_input, group_map, pool_scale)
    mix = jnp.zeros((own_rows, width), jnp.float32)
    for r, projection in zip(relative, projections):
        block = lax.dynamic_slice_in_dim(pieces, (lane ^ r) * own_rows, own_rows, axis=0)
        if r:
            block = across(block, "tp", r)
        mix = mix + jnp.dot(block, projection, preferred_element_type=jnp.float32)
    mixed = (resid.astype(jnp.float32) + mix).astype(jnp.bfloat16)
    residual = mixed.astype(jnp.float32)
    scaled = residual * lax.rsqrt(jnp.mean(residual * residual, axis=1, keepdims=True) + norm_eps)
    normed = (scaled * norm_gain.astype(jnp.float32)).astype(jnp.bfloat16)

    distance = (routes - lax.axis_index("sp") + experts) % experts
    named = distance[:, :, None] == jnp.arange(experts, dtype=jnp.int32)
    chosen = jnp.any(named, axis=1)
    ranks = jnp.dot(
        jnp.tril(jnp.ones((own_rows, own_rows), jnp.bfloat16), -1),
        chosen.astype(jnp.bfloat16),
        preferred_element_type=jnp.float32,
    ).astype(jnp.int32)
    weight = jnp.sum(jnp.where(named, route_weight[:, :, None], 0.0), axis=1)

    gate_w = expert_gate[0]
    up_w = expert_up[0]
    down_w = expert_down[0]
    per_step = experts <= lanes
    chunks = [[d] for d in range(experts)] if per_step else [list(range(experts))]
    sent = []
    for chunk in chunks:
        here = jnp.concatenate(
            [
                (ranks[:, d][:, None] == jnp.arange(slots, dtype=jnp.int32)) & chosen[:, d][:, None]
                for d in chunk
            ],
            axis=1,
        )
        rows = lax.dot_general(
            here.astype(jnp.bfloat16), normed, (((0,), (0,)), ((), ())),
            preferred_element_type=jnp.float32,
        ).astype(jnp.bfloat16)
        share = jnp.concatenate(
            [jnp.broadcast_to(weight[:, d][:, None], (own_rows, slots)) for d in chunk], axis=1
        )
        sent.append((rows, jnp.where(here, share, 0.0)))

    def out_to(d, rows):
        if per_step:
            return around(rows, "sp", d) if d else rows
        return swapped(rows)

    def back_from(d, rows):
        if per_step:
            return around(rows, "sp", -d) if d else rows
        return swapped(rows)

    def swapped(rows):
        first = lax.axis_index("sp")
        blocks = jnp.roll(rows.reshape(experts, -1), first, axis=0)
        blocks = lax.all_to_all(blocks, "sp", split_axis=0, concat_axis=0, tiled=True)
        return jnp.roll(blocks, -first, axis=0).reshape(rows.shape)

    total = residual
    for d, (rows, share) in enumerate(sent):
        parts = hypercube([out_to(d, rows)], "tp")
        own, kept, given = (expert_kernel if per_step else expert_block)(parts, gate_w, up_w, down_w)
        value = own
        bit = 1
        while bit < lanes:
            got = across(given, "tp", bit)
            value = value.astype(jnp.float32) + got[: value.shape[0]].astype(jnp.float32)
            value = value.astype(jnp.bfloat16)
            if kept.shape[0]:
                kept = kept.astype(jnp.float32) + got[own.shape[0] :].astype(jnp.float32)
                kept = kept.astype(jnp.bfloat16)
            half = (own.shape[0] + kept.shape[0]) // 2
            given = kept[half - own.shape[0] :]
            kept = kept[: half - own.shape[0]]
            bit *= 2
        back = back_from(d, value)
        high = share.astype(jnp.bfloat16)
        low = share - high.astype(jnp.float32)
        middle = low.astype(jnp.bfloat16)
        last = (low - middle.astype(jnp.float32)).astype(jnp.bfloat16)
        for part in (high, middle, last):
            total = total + jnp.dot(part, back, preferred_element_type=jnp.float32)
    return total.astype(jnp.bfloat16)


def solution(mesh):
    return jax.shard_map(
        local,
        mesh=mesh,
        in_specs=(
            P(("grp", "sp", "tp"), None),
            P(("grp", "sp"), "tp"),
            P("tp", None, None),
            P("tp"),
            P("tp", None),
            P(),
            P(("grp", "sp", "tp"), None),
            P(("grp", "sp", "tp"), None),
            P("sp", None, "tp"),
            P("sp", None, "tp"),
            P("sp", "tp", None),
        ),
        out_specs=P(("grp", "sp", "tp"), None),
        check_vma=False,
    )
```
